32 devices in a mesh: sp: 4 (over z), fs: 4 (over y, x), tp: 2 (over core).
Axes of the slice: x: 2, y: 2, z: 4, core: 2. Of those that a mesh axis runs over, the one named last changes fastest.
Arguments:
- tokens: bfloat16 [4, 8192, 2048], P('fs', 'sp'), may hold values from -21 to 21
- norm_gain: float32 [2048], replicated, may hold values from 0.1 to 1.9
- w_query: bfloat16 [2048, 1024], P(None, 'tp'), may hold values from -0.125 to 0.125
- w_key: bfloat16 [2048, 256], P(None, 'tp'), may hold values from -0.125 to 0.125
- w_value: bfloat16 [2048, 256], P(None, 'tp'), may hold values from -0.125 to 0.125
- w_pool: bfloat16 [2048, 1024], P(None, 'tp'), may hold values from -0.125 to 0.125
- w_group: bfloat16 [4, 256, 256], P('tp'), may hold values from -0.375 to 0.375
- w_out: bfloat16 [2048, 2048], replicated, may hold values from -0.125 to 0.125
- sinks: float32 [16], P('tp'), may hold values from -1 to 260
Outputs:
- mixed: bfloat16 [4, 8192, 2048], P('fs', ('sp', 'tp'))
- log_sums: float32 [4, 16, 8192], P('fs', 'tp', 'sp')
The draws below stay inside these ranges and needn't reach their ends.
All inputs are finite; a program needn't handle non-finite values.
Results may differ from the reference program's by a relative error of at most 0.009.
Values may be sent and summed in bfloat16 or wider, within the bound.
A program may use at most 192 MiB of HBM per device.

```python
import jax
import jax.numpy as jnp
from jax import lax

D = 2048
HEAD_SIZE = 64
QUERY_HEADS = 16
KEY_VALUE_HEADS = 4
GROUPS = 4
GDIM = 256
WINDOW_KEYS = 128
SEQS = 4
LEN = 8192
PW = 1024
QW = 1024
KW = 256


def draw_tokens(key, part):
    subkeys = jax.random.split(jax.random.fold_in(key, 11), 5)
    noise_part = jnp.clip(jax.random.normal(subkeys[0], (SEQS, LEN, D), jnp.float32), -4.0, 4.0)
    drift_sign = jnp.where(jax.random.uniform(subkeys[3], (SEQS, 1, 1), jnp.float32) < 0.5, -1.0, 1.0)
    drift_level = drift_sign * jax.random.uniform(subkeys[2], (SEQS, 1, 1), jnp.float32, 0.4, 1.0)
    rough_part = jax.random.uniform(subkeys[4], (SEQS, LEN // 32, 1), jnp.float32, -0.8, 0.8)
    direction = jnp.clip(jax.random.normal(subkeys[1], (SEQS, 1, D), jnp.float32), -3.0, 3.0)
    rise_factor = 1.0 + 2.0 * jnp.arange(LEN, dtype=jnp.float32)[None, :, None] / LEN
    amplitude = drift_level * rise_factor + jnp.repeat(rough_part, 32, axis=1)
    return (noise_part + amplitude * direction).astype(jnp.bfloat16)


def draw_sinks(key, part):
    subkeys = jax.random.split(jax.random.fold_in(key, 23), 1)
    sink_values = jax.random.uniform(subkeys[0], (QUERY_HEADS,), jnp.float32, -1.0, 6.0)
    return sink_values


def shard_levels(key, shape, pieces, smallest, high):
    factor_of, own = 1.0, jax.random.fold_in(key, 6)
    for position, shards_of in pieces:
        draws = jnp.exp(jax.random.uniform(jax.random.fold_in(own, position), (shards_of,), jnp.float32, smallest / len(pieces), high / len(pieces)))
        factor_of = factor_of * jnp.repeat(draws, shape[position] // shards_of).reshape([-1 if axis == position else 1 for axis in range(len(shape))])
    return factor_of


def scatter_about(stream_key, dims, width, bound, cuts=(), kind=jnp.bfloat16):
    entries = jax.random.normal(stream_key, dims, jnp.float32) * width
    if len(cuts) > 0:
        entries = shard_levels(stream_key, dims, cuts, -0.22, 0.18) * entries
    return jnp.clip(entries, min=-bound, max=bound).astype(kind)


def setup_inputs(seed: int = 0) -> dict:
    streams_of = jax.random.split(jax.random.key(seed), 10)
    return {
        "tokens": draw_tokens(jax.random.fold_in(streams_of[9], 71), 0),
        "norm_gain": jnp.clip(1.0 + 0.18 * jax.random.normal(streams_of[1], (D,), jnp.float32), 0.1, 1.9),
        "w_query": scatter_about(streams_of[2], (D, QW), D ** -0.5, 0.125, ((1, 2),)),
        "w_key": scatter_about(streams_of[3], (D, KW), D ** -0.5, 0.125, ((1, 2),)),
        "w_value": scatter_about(streams_of[4], (D, KW), D ** -0.5, 0.125, ((1, 2),)),
        "w_pool": scatter_about(streams_of[5], (D, PW), D ** -0.5, 0.125, ((1, 2),)),
        "w_group": scatter_about(streams_of[6], (GROUPS, GDIM, GDIM), GDIM ** -0.5, 0.375, ((0, 2),)),
        "w_out": scatter_about(streams_of[7], (PW + QW, D), (PW + QW) ** -0.5, 0.125),
        "sinks": draw_sinks(jax.random.fold_in(streams_of[9], 71), 0),
    }


LN_EPS = 1e-05

def normalize(token_rows, norm_gain):
    values = token_rows.astype(jnp.float32)
    row_mean = lax.optimization_barrier(jnp.mean(values, axis=-1, keepdims=True))
    centered = values - row_mean
    variance = lax.optimization_barrier(jnp.mean(centered * centered, axis=-1, keepdims=True))
    return (centered * lax.rsqrt(variance + LN_EPS) * norm_gain).astype(jnp.bfloat16)

def pool_branch(pool_rows, w_group):
    length = pool_rows.shape[0]
    reach = 2 ** GROUPS - 1
    values = pool_rows.astype(jnp.float32)
    padded = jnp.pad(values, ((reach, 0), (0, 0)))
    positions = jnp.arange(length, dtype=jnp.int32)
    prefix_mean = jnp.cumsum(values, axis=0) / (positions + 1).astype(jnp.float32)[:, None]
    outputs = []
    for group_index in range(GROUPS):
        span_width = 2 ** (group_index + 1)
        first_col = group_index * GDIM
        window_sum = jnp.zeros((length, GDIM), jnp.float32)
        for offset in range(span_width):
            window_sum = window_sum + padded[reach - offset:reach - offset + length, first_col:first_col + GDIM]
        window_count = jnp.minimum(positions + 1, span_width).astype(jnp.float32)[:, None]
        pooled = (window_sum / window_count - prefix_mean[:, first_col:first_col + GDIM]).astype(jnp.bfloat16)
        outputs.append(jnp.dot(pooled, w_group[group_index], preferred_element_type=jnp.float32).astype(jnp.bfloat16))
    return jnp.concatenate(outputs, axis=1)

def attention_branch(query_matrix, key_rows, value_rows, sinks):
    length = query_matrix.shape[0]
    block_extent = min(512, length)
    heads_per_group = QUERY_HEADS // KEY_VALUE_HEADS
    padded_keys = jnp.pad(key_rows, ((WINDOW_KEYS, 0), (0, 0)))
    padded_values = jnp.pad(value_rows, ((WINDOW_KEYS, 0), (0, 0)))
    attention_sink_logits = sinks.astype(jnp.float32).reshape(KEY_VALUE_HEADS, heads_per_group)[:, :, None, None]

    def one_block(block_index):
        start_row = (block_index * block_extent).astype(jnp.int32)
        query_tile_rows = lax.dynamic_slice_in_dim(query_matrix, start_row, block_extent, 0).reshape(block_extent, KEY_VALUE_HEADS, heads_per_group, HEAD_SIZE)
        key_tile_rows = lax.dynamic_slice_in_dim(padded_keys, start_row, block_extent + WINDOW_KEYS, 0).reshape(block_extent + WINDOW_KEYS, KEY_VALUE_HEADS, HEAD_SIZE)
        value_tile_rows = lax.dynamic_slice_in_dim(padded_values, start_row, block_extent + WINDOW_KEYS, 0).reshape(block_extent + WINDOW_KEYS, KEY_VALUE_HEADS, HEAD_SIZE)
        scores = jnp.einsum('qhrd,khd->hrqk', query_tile_rows.astype(jnp.float32), key_tile_rows.astype(jnp.float32)) * HEAD_SIZE ** (-0.5)
        query_positions = start_row + jnp.arange(block_extent, dtype=jnp.int32)
        key_positions = start_row - WINDOW_KEYS + jnp.arange(block_extent + WINDOW_KEYS, dtype=jnp.int32)
        distance = query_positions[:, None] - key_positions[None, :]
        visible = (distance >= 0) & (distance < WINDOW_KEYS) & (key_positions >= 0)[None, :]
        scores = jnp.where(visible, scores, -jnp.inf)
        row_max = jnp.maximum(lax.optimization_barrier(jnp.max(scores, axis=-1, keepdims=True)), attention_sink_logits)
        weights = jnp.exp(scores - row_max)
        weight_sum = lax.optimization_barrier(jnp.sum(weights, axis=-1, keepdims=True)) + jnp.exp(attention_sink_logits - row_max)
        normalized = (weights / weight_sum).astype(jnp.bfloat16)
        block_out = jnp.einsum('hrqk,khd->qhrd', normalized.astype(jnp.float32), value_tile_rows.astype(jnp.float32))
        block_out = block_out.astype(jnp.bfloat16).reshape(block_extent, QUERY_HEADS * HEAD_SIZE)
        block_logs = (row_max + jnp.log(weight_sum))[..., 0].reshape(QUERY_HEADS, block_extent)
        return (block_out, block_logs)
    block_outs, block_logs = lax.map(one_block, jnp.arange(length // block_extent, dtype=jnp.int32))
    attn_out = block_outs.reshape(length, QUERY_HEADS * HEAD_SIZE)
    log_sums = jnp.transpose(block_logs, (1, 0, 2)).reshape(QUERY_HEADS, length)
    return (attn_out, log_sums)

def reference(tokens, norm_gain, w_query, w_key, w_value, w_pool, w_group, w_out, sinks):

    def one_sequence(token_rows):
        normed = normalize(token_rows, norm_gain)
        query_matrix = jnp.dot(normed, w_query, preferred_element_type=jnp.float32).astype(jnp.bfloat16)
        key_rows = jnp.dot(normed, w_key, preferred_element_type=jnp.float32).astype(jnp.bfloat16)
        value_rows = jnp.dot(normed, w_value, preferred_element_type=jnp.float32).astype(jnp.bfloat16)
        pool_rows = jnp.dot(normed, w_pool, preferred_element_type=jnp.float32).astype(jnp.bfloat16)
        pool_out = pool_branch(pool_rows, w_group)
        attn_out, log_sums = attention_branch(query_matrix, key_rows, value_rows, sinks)
        joined = jnp.concatenate([pool_out, attn_out], axis=1)
        mixed = jnp.dot(joined, w_out, preferred_element_type=jnp.float32).astype(jnp.bfloat16)
        return (mixed, log_sums)
    mixed, log_sums = lax.map(one_sequence, tokens)
    return (mixed, log_sums)
```

```python
import functools

import jax
import jax.numpy as jnp
from jax import lax
from jax.experimental import pallas as pl
from jax.experimental.pallas import tpu as pltpu
from jax.sharding import PartitionSpec as P

HEAD_SIZE = 64
GDIM = 256
WINDOW = 128
LN_EPS = 1e-05
VMEM = 63 * 2**20
MESH = pl.DeviceIdType.MESH
BF = jnp.bfloat16
F32 = jnp.float32
NEG = -1e30


def dot(a, b, dims=((1,), (0,))):
    return lax.dot_general(a, b, (dims, ((), ())), preferred_element_type=F32)


def normalize(tok, gain, normed):
    width = tok.shape[1]

    def chunk(j):
        rows = slice(j * 64, (j + 1) * 64)
        x = tok[rows, :].astype(F32)
        centered = x - jnp.sum(x, axis=-1, keepdims=True) * (1.0 / width)
        variance = jnp.sum(centered * centered, axis=-1, keepdims=True) * (1.0 / width)
        normed[rows, :] = (centered * lax.rsqrt(variance + LN_EPS) * gain[...]).astype(BF)

    return [functools.partial(chunk, j) for j in range(tok.shape[0] // 64)]


def multiply(normed, wq, wk, wv, wp, q, kd, vt, pool, bsum, total, step):
    def do_q():
        q[...] = (dot(normed[...], wq[...]) * HEAD_SIZE**-0.5).astype(BF)

    def do_k():
        k = dot(normed[...], wk[...])
        rolled = pltpu.roll(k, HEAD_SIZE, 1)
        low = lax.broadcasted_iota(jnp.int32, k.shape, 1) < HEAD_SIZE
        kd[:, :WINDOW] = jnp.where(low, k, rolled).astype(BF)
        kd[:, WINDOW:] = jnp.where(low, rolled, k).astype(BF)

    def do_v():
        vt[...] = dot(normed[...], wv[...]).T.astype(BF)

    def do_p():
        p = dot(normed[...], wp[...]).astype(BF)
        pool[...] = p
        pf = p.astype(F32)
        sums = [
            jnp.sum(pf[b * WINDOW : (b + 1) * WINDOW], axis=0, keepdims=True)
            for b in range(p.shape[0] // WINDOW)
        ]
        tile_sum = functools.reduce(lambda a, b: a + b, sums)
        pad = jnp.zeros((8 - len(sums), pool.shape[1]), F32)
        bsum[0] = jnp.concatenate(sums + [pad], axis=0)
        total[...] = jnp.where(step > 1, total[...], 0.0) + tile_sum

    return [do_q, do_k, do_v, do_p]


def project_kernel(steps, tok, gain, wq, wk, wv, wp, q, kd, vt, pool, bsum, total, even, odd):
    step = pl.program_id(0)
    rest = (wq, wk, wv, wp, q, kd, vt, pool, bsum, total, step)

    @pl.when(step == 0)
    def _():
        for f in normalize(tok, gain, even):
            f()

    for parity in range(2):
        here, before = (even, odd) if parity == 0 else (odd, even)

        @pl.when((step > 0) & (step < steps) & (step % 2 == parity))
        def _():
            norms, mults = normalize(tok, gain, here), multiply(before, *rest)
            for n, m in zip(norms, mults):
                n()
                m()

    @pl.when(step == steps)
    def _():
        for f in multiply(odd if steps % 2 == 0 else even, *rest):
            f()


def project(tokens, gain, wq, wk, wv, wp):
    length, width = tokens.shape
    tile = 256
    steps = length // tile
    late = lambda i: jnp.maximum(i - 1, 0)
    qw, kw, pw = wq.shape[1], wk.shape[1], wp.shape[1]
    whole = lambda a: pl.BlockSpec(a.shape, lambda i: (0, 0), pipeline_mode=pl.Buffered(1))
    return pl.pallas_call(
        functools.partial(project_kernel, steps),
        grid=(steps + 1,),
        in_specs=[
            pl.BlockSpec((tile, width), lambda i: (jnp.minimum(i, steps - 1), 0)),
            whole(gain), whole(wq), whole(wk), whole(wv), whole(wp),
        ],
        out_specs=[
            pl.BlockSpec((tile, qw), lambda i: (late(i), 0)),
            pl.BlockSpec((tile, 2 * kw), lambda i: (late(i), 0)),
            pl.BlockSpec((kw, tile), lambda i: (0, late(i))),
            pl.BlockSpec((tile, pw), lambda i: (late(i), 0)),
            pl.BlockSpec((1, 8, pw), lambda i: (late(i), 0, 0)),
            pl.BlockSpec((1, pw), lambda i: (0, 0)),
        ],
        out_shape=[
            jax.ShapeDtypeStruct((length, qw), BF),
            jax.ShapeDtypeStruct((length, 2 * kw), BF),
            jax.ShapeDtypeStruct((kw, length), BF),
            jax.ShapeDtypeStruct((length, pw), BF),
            jax.ShapeDtypeStruct((steps, 8, pw), F32),
            jax.ShapeDtypeStruct((1, pw), F32),
        ],
        scratch_shapes=[pltpu.VMEM((tile, width), BF)] * 2,
        compiler_params=pltpu.CompilerParams(
            dimension_semantics=("arbitrary",), vmem_limit_bytes=VMEM
        ),
        cost_estimate=pl.CostEstimate(
            flops=2 * length * width * (qw + 2 * kw + pw),
            bytes_accessed=2 * length * width, transcendentals=0,
        ),
        name="project",
    )(tokens, gain, wq, wk, wv, wp)


def mix_kernel(
    mine, scal, q, kc, kp, vc, vp, pc, pp, khalo, vhalo, phalo, totals, bsum, wg, sinks, *outs
):
    out, logs = outs[-2:]
    step = pl.program_id(0)
    tp, sp, steps = scal[0], scal[1], scal[2]
    half = tp if mine else 1 - tp
    earlier = jnp.sum(totals[...], axis=0)
    first_step = half * pl.num_programs(0) + step
    tile = q.shape[0]
    at_start = first_step == 0
    keys = jnp.concatenate([jnp.where(at_start, khalo[...], kp[...]), kc[...]], axis=0)
    vals = jnp.concatenate([jnp.where(at_start, vhalo[...], vp[...]), vc[...]], axis=1)
    padded = jnp.concatenate(
        [jnp.zeros((WINDOW - phalo.shape[0], phalo.shape[1]), BF), phalo[...]], axis=0
    )
    rows = jnp.concatenate([jnp.where(at_start, padded, pp[...]), pc[...]], axis=0)
    lane = lax.broadcasted_iota(jnp.int32, (WINDOW, WINDOW), 1)
    low = (lane < HEAD_SIZE).astype(F32).astype(BF)
    high = (lane >= HEAD_SIZE).astype(F32).astype(BF)
    heads = 4
    key_id = lax.broadcasted_iota(jnp.int32, (WINDOW, heads * WINDOW), 0)
    query_id = lax.broadcasted_iota(jnp.int32, (WINDOW, heads * WINDOW), 1) % WINDOW
    seen = key_id <= query_id
    seen_f = seen.astype(F32).astype(BF)
    past_f = (key_id > query_id).astype(F32).astype(BF)
    nopast = jnp.logical_and(at_start, sp == 0)
    groups = wg.shape[0]
    drow = lax.broadcasted_iota(jnp.int32, (WINDOW, 2 * WINDOW), 0)
    dist = drow + WINDOW - lax.broadcasted_iota(jnp.int32, (WINDOW, 2 * WINDOW), 1)
    prefix = jnp.logical_and(dist >= 0, dist <= drow).astype(F32).astype(BF)
    blocks_per_sum = scal[3]
    sum_id = lax.broadcasted_iota(jnp.int32, bsum.shape, 0) * blocks_per_sum + (
        lax.broadcasted_iota(jnp.int32, bsum.shape, 1)
    )
    kvs = kc.shape[1] // WINDOW
    nblocks = tile // WINDOW
    sink_rows = [
        jnp.concatenate(
            [jnp.full((1, WINDOW), sinks[kv * heads + h], F32) for h in range(heads)], axis=1
        )
        for kv in range(kvs)
    ]

    def score(b, kv):
        parts = []
        for pair in range(2):
            c = (kv * 2 + pair) * WINDOW
            qp = q[b * WINDOW : (b + 1) * WINDOW, c : c + WINDOW]
            parts += [qp * low, qp * high]
        wr = slice(b * WINDOW, (b + 2) * WINDOW)
        return dot(
            keys[wr, kv * WINDOW : (kv + 1) * WINDOW], jnp.concatenate(parts, axis=0), ((1,), (1,))
        )

    def attend(b, kv, scores):
        br = slice(b * WINDOW, (b + 1) * WINDOW)
        past = scores[:WINDOW]
        if b == 0:
            past = past + jnp.where(nopast, F32(NEG), F32(0))
        picked = jnp.where(seen, scores[WINDOW:], past)
        sink = sink_rows[kv]
        row_max = jnp.maximum(jnp.max(picked, axis=0, keepdims=True), sink)
        weights = jnp.exp(picked - row_max)
        weight_sum = jnp.sum(weights, axis=0, keepdims=True) + jnp.exp(sink - row_max)
        log_row = row_max + jnp.log(weight_sum)
        for h in range(heads):
            logs[kv * heads + h : kv * heads + h + 1, br] = log_row[:, h * WINDOW : (h + 1) * WINDOW]
        wb = weights.astype(BF)
        stacked = jnp.concatenate([wb * past_f, wb * seen_f], axis=0)
        return stacked, 1.0 / weight_sum

    def collect(b, kv, stacked, scale):
        wr = slice(b * WINDOW, (b + 2) * WINDOW)
        o = dot(vals[kv * HEAD_SIZE : (kv + 1) * HEAD_SIZE, wr], stacked) * scale
        o = jnp.concatenate([o[:, h * WINDOW : (h + 1) * WINDOW] for h in range(heads)], axis=0)
        width = heads * HEAD_SIZE
        out[1, b * WINDOW : (b + 1) * WINDOW, kv * width : (kv + 1) * width] = o.astype(BF).T

    sum_row = lax.broadcasted_iota(jnp.int32, bsum.shape, 1)

    def pool_block(b, g):
        br = slice(b * WINDOW, (b + 1) * WINDOW)
        wr = slice(b * WINDOW, (b + 2) * WINDOW)
        cols = slice(g * GDIM, (g + 1) * GDIM)
        block = first_step * nblocks + b
        counted = jnp.logical_and(sum_id < block, sum_row < blocks_per_sum)[:, :, cols]
        carry = earlier[:, cols] + jnp.sum(
            jnp.sum(jnp.where(counted, bsum[:, :, cols], 0.0), axis=0), axis=0, keepdims=True
        )
        position = (
            sp * steps * tile + block * WINDOW
            + lax.broadcasted_iota(jnp.int32, (WINDOW, 1), 0) + 1
        )
        inv_pos = 1.0 / position.astype(F32)
        span = jnp.left_shift(jnp.int32(2), tp * groups + g)
        band = jnp.logical_and(dist >= 0, dist < span).astype(F32).astype(BF)
        sums = dot(jnp.concatenate([prefix, band], axis=0), rows[wr, cols])
        inv_count = 1.0 / jnp.minimum(position, span).astype(F32)
        pooled = (sums[WINDOW:] * inv_count - (sums[:WINDOW] + carry) * inv_pos).astype(BF)
        out[0, br, cols] = dot(pooled, wg[g]).astype(BF)

    units = [(b, kv) for b in range(nblocks) for kv in range(kvs)]
    pools = [(b, g) for b in range(nblocks) for g in range(groups)]
    scores = score(*units[0])
    pending = None
    for u, unit in enumerate(units):
        later = score(*units[u + 1]) if u + 1 < len(units) else None
        if pending is not None:
            collect(*pending)
        if u < len(pools):
            pool_block(*pools[u])
        pending = (*unit, *attend(*unit, scores))
        scores = later
    collect(*pending)
    for extra in pools[len(units) :]:
        pool_block(*extra)


def mix(mine, scal, q, kd, vt, pool, khalo, vhalo, phalo, totals, bsum, wg, sinks, *logs_in):
    length, qw = q.shape
    tile = 256
    per = tile // WINDOW
    steps = length // tile // 2
    pw = pool.shape[1]
    heads = sinks.shape[0]
    half = lambda s: s[0] if mine else 1 - s[0]
    cur = lambda i, s: half(s) * steps + i
    prev = lambda i, s: jnp.maximum(cur(i, s) * per - 1, 0)
    whole = lambda a: pl.BlockSpec(a.shape, lambda i, s: (0,) * a.ndim)
    return pl.pallas_call(
        functools.partial(mix_kernel, mine),
        grid_spec=pltpu.PrefetchScalarGridSpec(
            num_scalar_prefetch=1,
            grid=(steps,),
            in_specs=[
                pl.BlockSpec((tile, qw), lambda i, s: (cur(i, s), 0)),
                pl.BlockSpec((tile, kd.shape[1]), lambda i, s: (cur(i, s), 0)),
                pl.BlockSpec((WINDOW, kd.shape[1]), lambda i, s: (prev(i, s), 0)),
                pl.BlockSpec((vt.shape[0], tile), lambda i, s: (0, cur(i, s))),
                pl.BlockSpec((vt.shape[0], WINDOW), lambda i, s: (0, prev(i, s))),
                pl.BlockSpec((tile, pw), lambda i, s: (cur(i, s), 0)),
                pl.BlockSpec((WINDOW, pw), lambda i, s: (prev(i, s), 0)),
                whole(khalo), whole(vhalo), whole(phalo), whole(totals), whole(bsum), whole(wg),
                pl.BlockSpec(memory_space=pltpu.SMEM),
            ]
            + [pl.BlockSpec(memory_space=pl.ANY)] * len(logs_in),
            out_specs=[
                pl.BlockSpec((2, tile, qw), lambda i, s: (0, i, 0)),
                pl.BlockSpec((heads, tile), lambda i, s: (0, cur(i, s))),
            ],
        ),
        out_shape=[
            jax.ShapeDtypeStruct((2, length // 2, qw), BF),
            jax.ShapeDtypeStruct((heads, length), F32),
        ],
        input_output_aliases={15: 1} if logs_in else {},
        compiler_params=pltpu.CompilerParams(
            dimension_semantics=("arbitrary",), vmem_limit_bytes=VMEM
        ),
        cost_estimate=pl.CostEstimate(
            flops=length // 2 * 2 * qw * 1024, bytes_accessed=length * qw * 4,
            transcendentals=length // 2 * 1024,
        ),
        name="mix",
    )(scal, q, kd, kd, vt, vt, pool, pool, khalo, vhalo, phalo, totals, bsum, wg, sinks, *logs_in)


def share_kernel(count, kd, vt, pool, total, khalo, vhalo, phalo, totals, send, recv, tsend, trecv):
    me = lax.axis_index("sp")
    length = kd.shape[0]
    totals[...] = jnp.zeros_like(totals)
    barrier = pltpu.get_barrier_semaphore()
    for hop in range(1, count):
        pl.semaphore_signal(
            barrier, inc=1, device_id={"sp": lax.rem(me + hop, count)}, device_id_type=MESH
        )
    first = me == 0

    @pl.when(first)
    def _():
        khalo[...] = jnp.zeros_like(khalo)
        vhalo[...] = jnp.zeros_like(vhalo)
        phalo[...] = jnp.zeros_like(phalo)

    pl.semaphore_wait(barrier, count - 1)
    right = {"sp": lax.rem(me + 1, count)}
    pairs = (
        (kd.at[pl.ds(length - WINDOW, WINDOW), :], khalo),
        (vt.at[:, pl.ds(length - WINDOW, WINDOW)], vhalo),
        (pool.at[pl.ds(length - 16, 16), :], phalo),
    )
    halos = [
        pltpu.make_async_remote_copy(
            src_ref=src, dst_ref=dst, send_sem=send.at[j], recv_sem=recv.at[j],
            device_id=right, device_id_type=MESH,
        )
        for j, (src, dst) in enumerate(pairs)
    ]

    def sum_copy(hop):
        return pltpu.make_async_remote_copy(
            src_ref=total, dst_ref=totals.at[hop], send_sem=tsend.at[hop],
            recv_sem=trecv.at[hop], device_id={"sp": lax.rem(me + hop, count)},
            device_id_type=MESH,
        )

    @pl.when(me < count - 1)
    def _():
        for copy in halos:
            copy.start()

    for hop in range(1, count):

        @pl.when(me + hop < count)
        def _():
            sum_copy(hop).start()

    @pl.when(me > 0)
    def _():
        for copy in halos:
            copy.wait_recv()

    @pl.when(me < count - 1)
    def _():
        for copy in halos:
            copy.wait_send()

    for hop in range(1, count):

        @pl.when(me >= hop)
        def _():
            sum_copy(hop).wait_recv()

        @pl.when(me + hop < count)
        def _():
            sum_copy(hop).wait_send()


def share(kd, vt, pool, total):
    count = lax.axis_size("sp")
    vmem = pl.BlockSpec(memory_space=pltpu.VMEM)
    return pl.pallas_call(
        functools.partial(share_kernel, count),
        in_specs=[pl.BlockSpec(memory_space=pl.ANY)] * 3 + [vmem],
        out_specs=[vmem] * 4,
        out_shape=[
            jax.ShapeDtypeStruct((WINDOW, kd.shape[1]), BF),
            jax.ShapeDtypeStruct((vt.shape[0], WINDOW), BF),
            jax.ShapeDtypeStruct((16, pool.shape[1]), BF),
            jax.ShapeDtypeStruct((count, *total.shape), F32),
        ],
        scratch_shapes=[
            pltpu.SemaphoreType.DMA((3,)),
            pltpu.SemaphoreType.DMA((3,)),
            pltpu.SemaphoreType.DMA((count,)),
            pltpu.SemaphoreType.DMA((count,)),
        ],
        compiler_params=pltpu.CompilerParams(
            collective_id=0, has_side_effects=True, vmem_limit_bytes=VMEM
        ),
        name="share",
    )(kd, vt, pool, total)


def output_kernel(scal, own, other, w, out):
    tp = scal[0]
    width = own.shape[2]
    acc = None
    for kind in range(2):
        for x, who in ((own, tp), (other, 1 - tp)):
            start = pl.multiple_of((kind * 2 + who) * width, width)
            part = dot(x[kind], w[pl.ds(start, width), :])
            acc = part if acc is None else acc + part
    out[...] = acc.astype(BF)


def output(scal, own, other, w):
    rows, width = own.shape[1:]
    cols = w.shape[1]
    tile = 256
    return pl.pallas_call(
        output_kernel,
        grid_spec=pltpu.PrefetchScalarGridSpec(
            num_scalar_prefetch=1,
            grid=(cols // tile,),
            in_specs=[
                pl.BlockSpec(own.shape, lambda i, s: (0, 0, 0), pipeline_mode=pl.Buffered(1)),
                pl.BlockSpec(own.shape, lambda i, s: (0, 0, 0), pipeline_mode=pl.Buffered(1)),
                pl.BlockSpec((w.shape[0], tile), lambda i, s: (0, i)),
            ],
            out_specs=pl.BlockSpec((rows, tile), lambda i, s: (0, i)),
        ),
        out_shape=jax.ShapeDtypeStruct((rows, cols), BF),
        compiler_params=pltpu.CompilerParams(
            dimension_semantics=("arbitrary",), vmem_limit_bytes=VMEM
        ),
        cost_estimate=pl.CostEstimate(
            flops=2 * rows * w.shape[0] * cols, bytes_accessed=2 * w.size, transcendentals=0
        ),
        name="output",
    )(scal, own, other, w)


def body(tokens, norm_gain, w_query, w_key, w_value, w_pool, w_group, w_out, sinks):
    q, kd, vt, pool, bsum, total = project(
        tokens[0], norm_gain[None, :], w_query, w_key, w_value, w_pool
    )
    length = q.shape[0]
    halos = share(kd, vt, pool, total)
    per_sum = length // bsum.shape[0] // WINDOW
    scal = jnp.stack(
        [lax.axis_index("tp"), lax.axis_index("sp"), jnp.int32(length // 256), jnp.int32(per_sum)]
    ).astype(jnp.int32)
    shared = (scal, q, kd, vt, pool, *halos, bsum, w_group, sinks)
    theirs, logs = mix(False, *shared)
    other = lax.ppermute(theirs, "tp", [(0, 1), (1, 0)])
    own, logs = mix(True, *shared, logs)
    return (output(scal, own, other, w_out)[None], logs[None])


def solution(mesh):
    return jax.shard_map(
        body,
        mesh=mesh,
        in_specs=(
            P("fs", "sp", None),
            P(),
            P(None, "tp"),
            P(None, "tp"),
            P(None, "tp"),
            P(None, "tp"),
            P("tp", None, None),
            P(),
            P("tp"),
        ),
        out_specs=(P("fs", ("sp", "tp"), None), P("fs", "tp", "sp")),
        check_vma=False,
    )
```

```python
import functools

import jax
import jax.numpy as jnp
from jax import lax
from jax.experimental import pallas as pl
from jax.experimental.pallas import tpu as pltpu
from jax.sharding import PartitionSpec as P

HEAD_SIZE = 64
GDIM = 256
WINDOW = 128
LN_EPS = 1e-05
SUB = 256
VMEM = 63 * 2**20
MESH = pl.DeviceIdType.MESH
BF = jnp.bfloat16
F32 = jnp.float32
NEG = -1e30


def dot(a, b, dims=((1,), (0,))):
    return lax.dot_general(a, b, (dims, ((), ())), preferred_element_type=F32)


def project_kernel(subs, tok, gain, wq, wk, wv, wp, q, kd, vt, pool, bsum, total):
    step = pl.program_id(0)
    width = tok.shape[1]
    rows_sums = []
    for s in range(subs):
        rows = slice(s * SUB, (s + 1) * SUB)
        x = tok[rows, :].astype(F32)
        centered = x - jnp.sum(x, axis=-1, keepdims=True) * (1.0 / width)
        variance = jnp.sum(centered * centered, axis=-1, keepdims=True) * (1.0 / width)
        normed = (centered * lax.rsqrt(variance + LN_EPS) * gain[...]).astype(BF)
        q[rows, :] = (dot(normed, wq[...]) * HEAD_SIZE**-0.5).astype(BF)
        k = dot(normed, wk[...])
        rolled = pltpu.roll(k, HEAD_SIZE, 1)
        low = lax.broadcasted_iota(jnp.int32, k.shape, 1) < HEAD_SIZE
        kd[rows, :WINDOW] = jnp.where(low, k, rolled).astype(BF)
        kd[rows, WINDOW:] = jnp.where(low, rolled, k).astype(BF)
        vt[:, rows] = dot(normed, wv[...]).T.astype(BF)
        p = dot(normed, wp[...]).astype(BF)
        pool[rows, :] = p
        pf = p.astype(F32)
        for b in range(SUB // WINDOW):
            rows_sums.append(
                jnp.sum(pf[b * WINDOW : (b + 1) * WINDOW], axis=0, keepdims=True)
            )
    tile_sum = functools.reduce(lambda a, b: a + b, rows_sums)
    pad = jnp.zeros((8 - len(rows_sums), pool.shape[1]), F32)
    bsum[0] = jnp.concatenate(rows_sums + [pad], axis=0)

    @pl.when(step == 0)
    def _():
        total[...] = tile_sum

    @pl.when(step > 0)
    def _():
        total[...] += tile_sum


def project(tokens, gain, wq, wk, wv, wp):
    length, width = tokens.shape
    tile = 512
    steps = length // tile
    qw, kw, pw = wq.shape[1], wk.shape[1], wp.shape[1]
    whole = lambda a: pl.BlockSpec(a.shape, lambda i: (0, 0), pipeline_mode=pl.Buffered(1))
    return pl.pallas_call(
        functools.partial(project_kernel, tile // SUB),
        grid=(steps,),
        in_specs=[
            pl.BlockSpec((tile, width), lambda i: (i, 0)),
            whole(gain), whole(wq), whole(wk), whole(wv), whole(wp),
        ],
        out_specs=[
            pl.BlockSpec((tile, qw), lambda i: (i, 0)),
            pl.BlockSpec((tile, 2 * kw), lambda i: (i, 0)),
            pl.BlockSpec((kw, tile), lambda i: (0, i)),
            pl.BlockSpec((tile, pw), lambda i: (i, 0)),
            pl.BlockSpec((1, 8, pw), lambda i: (i, 0, 0)),
            pl.BlockSpec((1, pw), lambda i: (0, 0)),
        ],
        out_shape=[
            jax.ShapeDtypeStruct((length, qw), BF),
            jax.ShapeDtypeStruct((length, 2 * kw), BF),
            jax.ShapeDtypeStruct((kw, length), BF),
            jax.ShapeDtypeStruct((length, pw), BF),
            jax.ShapeDtypeStruct((steps, 8, pw), F32),
            jax.ShapeDtypeStruct((1, pw), F32),
        ],
        compiler_params=pltpu.CompilerParams(
            dimension_semantics=("arbitrary",), vmem_limit_bytes=VMEM
        ),
        cost_estimate=pl.CostEstimate(
            flops=2 * length * width * (qw + 2 * kw + pw),
            bytes_accessed=2 * length * width, transcendentals=0,
        ),
        name="project",
    )(tokens, gain, wq, wk, wv, wp)


def mix_kernel(
    mine, scal, q, kc, kp, vc, vp, pc, pp, khalo, vhalo, phalo, totals, bsum, wg, sinks, *outs
):
    out, logs = outs[-2:]
    step = pl.program_id(0)
    tp, sp, steps = scal[0], scal[1], scal[2]
    half = tp if mine else 1 - tp
    earlier = jnp.sum(totals[...], axis=0)
    first_step = half * pl.num_programs(0) + step
    tile = q.shape[0]
    at_start = first_step == 0
    keys = jnp.concatenate([jnp.where(at_start, khalo[...], kp[...]), kc[...]], axis=0)
    vals = jnp.concatenate([jnp.where(at_start, vhalo[...], vp[...]), vc[...]], axis=1)
    padded = jnp.concatenate(
        [jnp.zeros((WINDOW - phalo.shape[0], phalo.shape[1]), BF), phalo[...]], axis=0
    )
    rows = jnp.concatenate([jnp.where(at_start, padded, pp[...]), pc[...]], axis=0)
    lane = lax.broadcasted_iota(jnp.int32, (WINDOW, WINDOW), 1)
    low = (lane < HEAD_SIZE).astype(F32).astype(BF)
    high = (lane >= HEAD_SIZE).astype(F32).astype(BF)
    heads = 4
    key_id = lax.broadcasted_iota(jnp.int32, (WINDOW, heads * WINDOW), 0)
    query_id = lax.broadcasted_iota(jnp.int32, (WINDOW, heads * WINDOW), 1) % WINDOW
    seen = key_id <= query_id
    seen_f = seen.astype(F32).astype(BF)
    past_f = (key_id > query_id).astype(F32).astype(BF)
    nopast = jnp.logical_and(at_start, sp == 0)
    groups = wg.shape[0]
    drow = lax.broadcasted_iota(jnp.int32, (WINDOW, 2 * WINDOW), 0)
    dist = drow + WINDOW - lax.broadcasted_iota(jnp.int32, (WINDOW, 2 * WINDOW), 1)
    prefix = jnp.logical_and(dist >= 0, dist <= drow).astype(F32).astype(BF)
    blocks_per_sum = scal[3]
    sum_id = lax.broadcasted_iota(jnp.int32, bsum.shape, 0) * blocks_per_sum + (
        lax.broadcasted_iota(jnp.int32, bsum.shape, 1)
    )
    kvs = kc.shape[1] // WINDOW
    nblocks = tile // WINDOW
    sink_rows = [
        jnp.concatenate(
            [jnp.full((1, WINDOW), sinks[kv * heads + h], F32) for h in range(heads)], axis=1
        )
        for kv in range(kvs)
    ]

    def score(b, kv):
        parts = []
        for pair in range(2):
            c = (kv * 2 + pair) * WINDOW
            qp = q[b * WINDOW : (b + 1) * WINDOW, c : c + WINDOW]
            parts += [qp * low, qp * high]
        wr = slice(b * WINDOW, (b + 2) * WINDOW)
        return dot(
            keys[wr, kv * WINDOW : (kv + 1) * WINDOW], jnp.concatenate(parts, axis=0), ((1,), (1,))
        )

    def attend(b, kv, scores):
        br = slice(b * WINDOW, (b + 1) * WINDOW)
        past = scores[:WINDOW]
        if b == 0:
            past = past + jnp.where(nopast, F32(NEG), F32(0))
        picked = jnp.where(seen, scores[WINDOW:], past)
        sink = sink_rows[kv]
        row_max = jnp.maximum(jnp.max(picked, axis=0, keepdims=True), sink)
        weights = jnp.exp(picked - row_max)
        weight_sum = jnp.sum(weights, axis=0, keepdims=True) + jnp.exp(sink - row_max)
        log_row = row_max + jnp.log(weight_sum)
        for h in range(heads):
            logs[kv * heads + h : kv * heads + h + 1, br] = log_row[:, h * WINDOW : (h + 1) * WINDOW]
        wb = weights.astype(BF)
        stacked = jnp.concatenate([wb * past_f, wb * seen_f], axis=0)
        return stacked, 1.0 / weight_sum

    def collect(b, kv, stacked, scale):
        wr = slice(b * WINDOW, (b + 2) * WINDOW)
        o = dot(vals[kv * HEAD_SIZE : (kv + 1) * HEAD_SIZE, wr], stacked) * scale
        o = jnp.concatenate([o[:, h * WINDOW : (h + 1) * WINDOW] for h in range(heads)], axis=0)
        width = heads * HEAD_SIZE
        out[1, b * WINDOW : (b + 1) * WINDOW, kv * width : (kv + 1) * width] = o.astype(BF).T

    sum_row = lax.broadcasted_iota(jnp.int32, bsum.shape, 1)

    def pool_block(b, g):
        br = slice(b * WINDOW, (b + 1) * WINDOW)
        wr = slice(b * WINDOW, (b + 2) * WINDOW)
        cols = slice(g * GDIM, (g + 1) * GDIM)
        block = first_step * nblocks + b
        counted = jnp.logical_and(sum_id < block, sum_row < blocks_per_sum)[:, :, cols]
        carry = earlier[:, cols] + jnp.sum(
            jnp.sum(jnp.where(counted, bsum[:, :, cols], 0.0), axis=0), axis=0, keepdims=True
        )
        position = (
            sp * steps * tile + block * WINDOW
            + lax.broadcasted_iota(jnp.int32, (WINDOW, 1), 0) + 1
        )
        inv_pos = 1.0 / position.astype(F32)
        span = jnp.left_shift(jnp.int32(2), tp * groups + g)
        band = jnp.logical_and(dist >= 0, dist < span).astype(F32).astype(BF)
        sums = dot(jnp.concatenate([prefix, band], axis=0), rows[wr, cols])
        inv_count = 1.0 / jnp.minimum(position, span).astype(F32)
        pooled = (sums[WINDOW:] * inv_count - (sums[:WINDOW] + carry) * inv_pos).astype(BF)
        out[0, br, cols] = dot(pooled, wg[g]).astype(BF)

    units = [(b, kv) for b in range(nblocks) for kv in range(kvs)]
    pools = [(b, g) for b in range(nblocks) for g in range(groups)]
    scores = score(*units[0])
    pending = None
    for u, unit in enumerate(units):
        later = score(*units[u + 1]) if u + 1 < len(units) else None
        if pending is not None:
            collect(*pending)
        if u < len(pools):
            pool_block(*pools[u])
        pending = (*unit, *attend(*unit, scores))
        scores = later
    collect(*pending)
    for extra in pools[len(units) :]:
        pool_block(*extra)


def mix(mine, scal, q, kd, vt, pool, khalo, vhalo, phalo, totals, bsum, wg, sinks, *logs_in):
    length, qw = q.shape
    tile = 256
    per = tile // WINDOW
    steps = length // tile // 2
    pw = pool.shape[1]
    heads = sinks.shape[0]
    half = lambda s: s[0] if mine else 1 - s[0]
    cur = lambda i, s: half(s) * steps + i
    prev = lambda i, s: jnp.maximum(cur(i, s) * per - 1, 0)
    whole = lambda a: pl.BlockSpec(a.shape, lambda i, s: (0,) * a.ndim)
    return pl.pallas_call(
        functools.partial(mix_kernel, mine),
        grid_spec=pltpu.PrefetchScalarGridSpec(
            num_scalar_prefetch=1,
            grid=(steps,),
            in_specs=[
                pl.BlockSpec((tile, qw), lambda i, s: (cur(i, s), 0)),
                pl.BlockSpec((tile, kd.shape[1]), lambda i, s: (cur(i, s), 0)),
                pl.BlockSpec((WINDOW, kd.shape[1]), lambda i, s: (prev(i, s), 0)),
                pl.BlockSpec((vt.shape[0], tile), lambda i, s: (0, cur(i, s))),
                pl.BlockSpec((vt.shape[0], WINDOW), lambda i, s: (0, prev(i, s))),
                pl.BlockSpec((tile, pw), lambda i, s: (cur(i, s), 0)),
                pl.BlockSpec((WINDOW, pw), lambda i, s: (prev(i, s), 0)),
                whole(khalo), whole(vhalo), whole(phalo), whole(totals), whole(bsum), whole(wg),
                pl.BlockSpec(memory_space=pltpu.SMEM),
            ]
            + [pl.BlockSpec(memory_space=pl.ANY)] * len(logs_in),
            out_specs=[
                pl.BlockSpec((2, tile, qw), lambda i, s: (0, i, 0)),
                pl.BlockSpec((heads, tile), lambda i, s: (0, cur(i, s))),
            ],
        ),
        out_shape=[
            jax.ShapeDtypeStruct((2, length // 2, qw), BF),
            jax.ShapeDtypeStruct((heads, length), F32),
        ],
        input_output_aliases={15: 1} if logs_in else {},
        compiler_params=pltpu.CompilerParams(
            dimension_semantics=("arbitrary",), vmem_limit_bytes=VMEM
        ),
        cost_estimate=pl.CostEstimate(
            flops=length // 2 * 2 * qw * 1024, bytes_accessed=length * qw * 4,
            transcendentals=length // 2 * 1024,
        ),
        name="mix",
    )(scal, q, kd, kd, vt, vt, pool, pool, khalo, vhalo, phalo, totals, bsum, wg, sinks, *logs_in)


def share_kernel(count, kd, vt, pool, total, khalo, vhalo, phalo, totals, send, recv, tsend, trecv):
    me = lax.axis_index("sp")
    length = kd.shape[0]
    totals[...] = jnp.zeros_like(totals)
    barrier = pltpu.get_barrier_semaphore()
    for hop in range(1, count):
        pl.semaphore_signal(
            barrier, inc=1, device_id={"sp": lax.rem(me + hop, count)}, device_id_type=MESH
        )
    first = me == 0

    @pl.when(first)
    def _():
        khalo[...] = jnp.zeros_like(khalo)
        vhalo[...] = jnp.zeros_like(vhalo)
        phalo[...] = jnp.zeros_like(phalo)

    pl.semaphore_wait(barrier, count - 1)
    right = {"sp": lax.rem(me + 1, count)}
    pairs = (
        (kd.at[pl.ds(length - WINDOW, WINDOW), :], khalo),
        (vt.at[:, pl.ds(length - WINDOW, WINDOW)], vhalo),
        (pool.at[pl.ds(length - 16, 16), :], phalo),
    )
    halos = [
        pltpu.make_async_remote_copy(
            src_ref=src, dst_ref=dst, send_sem=send.at[j], recv_sem=recv.at[j],
            device_id=right, device_id_type=MESH,
        )
        for j, (src, dst) in enumerate(pairs)
    ]

    def sum_copy(hop):
        return pltpu.make_async_remote_copy(
            src_ref=total, dst_ref=totals.at[hop], send_sem=tsend.at[hop],
            recv_sem=trecv.at[hop], device_id={"sp": lax.rem(me + hop, count)},
            device_id_type=MESH,
        )

    @pl.when(me < count - 1)
    def _():
        for copy in halos:
            copy.start()

    for hop in range(1, count):

        @pl.when(me + hop < count)
        def _():
            sum_copy(hop).start()

    @pl.when(me > 0)
    def _():
        for copy in halos:
            copy.wait_recv()

    @pl.when(me < count - 1)
    def _():
        for copy in halos:
            copy.wait_send()

    for hop in range(1, count):

        @pl.when(me >= hop)
        def _():
            sum_copy(hop).wait_recv()

        @pl.when(me + hop < count)
        def _():
            sum_copy(hop).wait_send()


def share(kd, vt, pool, total):
    count = lax.axis_size("sp")
    vmem = pl.BlockSpec(memory_space=pltpu.VMEM)
    return pl.pallas_call(
        functools.partial(share_kernel, count),
        in_specs=[pl.BlockSpec(memory_space=pl.ANY)] * 3 + [vmem],
        out_specs=[vmem] * 4,
        out_shape=[
            jax.ShapeDtypeStruct((WINDOW, kd.shape[1]), BF),
            jax.ShapeDtypeStruct((vt.shape[0], WINDOW), BF),
            jax.ShapeDtypeStruct((16, pool.shape[1]), BF),
            jax.ShapeDtypeStruct((count, *total.shape), F32),
        ],
        scratch_shapes=[
            pltpu.SemaphoreType.DMA((3,)),
            pltpu.SemaphoreType.DMA((3,)),
            pltpu.SemaphoreType.DMA((count,)),
            pltpu.SemaphoreType.DMA((count,)),
        ],
        compiler_params=pltpu.CompilerParams(
            collective_id=0, has_side_effects=True, vmem_limit_bytes=VMEM
        ),
        name="share",
    )(kd, vt, pool, total)


def output_kernel(own, other, w, out, joined, sems):
    width = own.shape[2]

    @pl.when(pl.program_id(0) == 0)
    def _():
        tp = lax.axis_index("tp")
        copies = []
        for kind in range(2):
            for j, (x, who) in enumerate(((own, tp), (other, 1 - tp))):
                start = pl.multiple_of((kind * 2 + who) * width, width)
                copies.append(
                    pltpu.make_async_copy(
                        x.at[kind], joined.at[:, pl.ds(start, width)], sems.at[kind * 2 + j]
                    )
                )
        for copy in copies:
            copy.start()
        for copy in copies:
            copy.wait()

    out[...] = dot(joined[...], w[...]).astype(BF)


def output(own, other, w):
    rows = own.shape[1]
    depth, cols = w.shape
    tile = 512
    return pl.pallas_call(
        output_kernel,
        grid=(cols // tile,),
        in_specs=[
            pl.BlockSpec(memory_space=pl.ANY),
            pl.BlockSpec(memory_space=pl.ANY),
            pl.BlockSpec((depth, tile), lambda i: (0, i)),
        ],
        out_specs=pl.BlockSpec((rows, tile), lambda i: (0, i)),
        out_shape=jax.ShapeDtypeStruct((rows, cols), BF),
        scratch_shapes=[pltpu.VMEM((rows, depth), BF), pltpu.SemaphoreType.DMA((4,))],
        compiler_params=pltpu.CompilerParams(
            dimension_semantics=("arbitrary",), vmem_limit_bytes=VMEM
        ),
        cost_estimate=pl.CostEstimate(
            flops=2 * rows * depth * cols, bytes_accessed=2 * w.size, transcendentals=0
        ),
        name="output",
    )(own, other, w)


def body(tokens, norm_gain, w_query, w_key, w_value, w_pool, w_group, w_out, sinks):
    q, kd, vt, pool, bsum, total = project(
        tokens[0], norm_gain[None, :], w_query, w_key, w_value, w_pool
    )
    length = q.shape[0]
    halos = share(kd, vt, pool, total)
    per_sum = length // bsum.shape[0] // WINDOW
    scal = jnp.stack(
        [lax.axis_index("tp"), lax.axis_index("sp"), jnp.int32(length // 256), jnp.int32(per_sum)]
    ).astype(jnp.int32)
    shared = (scal, q, kd, vt, pool, *halos, bsum, w_group, sinks)
    theirs, logs = mix(False, *shared)
    other = lax.ppermute(theirs, "tp", [(0, 1), (1, 0)])
    own, logs = mix(True, *shared, logs)
    return (output(own, other, w_out)[None], logs[None])


def solution(mesh):
    return jax.shard_map(
        body,
        mesh=mesh,
        in_specs=(
            P("fs", "sp", None),
            P(),
            P(None, "tp"),
            P(None, "tp"),
            P(None, "tp"),
            P(None, "tp"),
            P("tp", None, None),
            P(),
            P("tp"),
        ),
        out_specs=(P("fs", ("sp", "tp"), None), P("fs", "tp", "sp")),
        check_vma=False,
    )
```
